32 devices in a mesh: fs: 16 (over z, y, x), tp: 2 (over core).
Axes of the slice: x: 2, y: 2, z: 4, core: 2. Of those that a mesh axis runs over, the one named last changes fastest.
Arguments:
- saved_inputs: bfloat16 [12288, 2048], P('fs'), may hold values from -8 to 8
- input_cot: bfloat16 [12288, 2048], P('fs', 'tp'), may hold values from -0.0546875 to 0.0546875
- gate_cot: bfloat16 [12288, 2048], P('fs', 'tp'), may hold values from -0.0546875 to 0.0546875
- input_master: float32 [2048, 2048], P('fs', 'tp'), may hold values from -6 to 6
- gate_master: float32 [2048, 2048], P('fs', 'tp'), may hold values from -6 to 6
- input_factor: bfloat16 [2048, 256], P('fs'), may hold values from -2 to 2
- gate_factor: bfloat16 [2048, 256], P('fs'), may hold values from -2 to 2
- input_first: float32 [256, 2048], P('fs', 'tp'), may hold values from -6 to 6
- input_second: float32 [256, 2048], P('fs', 'tp'), may hold values from 0.2 to 17
- gate_first: float32 [256, 2048], P('fs', 'tp'), may hold values from -6 to 6
- gate_second: float32 [256, 2048], P('fs', 'tp'), may hold values from 0.2 to 17
Outputs:
- input_step: float32 [2048, 2048], P('fs', 'tp')
- gate_step: float32 [2048, 2048], P('fs', 'tp')
- input_first_new: float32 [256, 2048], P('fs', 'tp')
- input_second_new: float32 [256, 2048], P('fs', 'tp')
- gate_first_new: float32 [256, 2048], P('fs', 'tp')
- gate_second_new: float32 [256, 2048], P('fs', 'tp')
- input_copy: bfloat16 [2048, 2048], P(None, 'tp')
- gate_copy: bfloat16 [2048, 2048], P(None, 'tp')
The draws below stay inside these ranges and needn't reach their ends.
All inputs are finite; a program needn't handle non-finite values.
Results may differ from the reference program's by a relative error of at most 0.0004.
Values may be sent and summed in bfloat16 or wider, within the bound.
A program may use at most 64 MiB of HBM per device.

```python
import jax
import jax.numpy as jnp
from jax import lax

D = 2048
W = 2048
RANK = 256
TOKENS = 12288


def factor_draw(key, salt):
    keyed = jax.random.fold_in(key, salt)
    key_one, key_two = jax.random.split(keyed)
    position = jnp.arange(D, dtype=jnp.float32)[:, None] / D
    jitter = jnp.exp(jax.random.uniform(key_one, (D, 1), jnp.float32, -0.7, 0.7))
    scales = jnp.exp(jnp.log(6.0) * position) * jitter / 2.8
    entries = jax.random.normal(key_two, (D, RANK), jnp.float32)
    values = jnp.clip(entries * scales * D ** (-0.5), -2.0, 2.0)
    return values.astype(jnp.bfloat16)


def second_draw(key, salt):
    keyed = jax.random.fold_in(key, salt)
    column = jnp.arange(W, dtype=jnp.float32)[None, :] / W
    jitter = jnp.exp(jax.random.uniform(keyed, (RANK, W), jnp.float32, -0.7, 0.7))
    spread = jnp.exp(jnp.log(9.0) * (1.0 - column))
    return (0.5 * jitter * spread).astype(jnp.float32)


def draw_input_factor(key, part):
    return factor_draw(key, 11)


def draw_gate_factor(key, part):
    return factor_draw(key, 23)


def draw_input_second(key, part):
    return second_draw(key, 37)


def draw_gate_second(key, part):
    return second_draw(key, 41)


def raised(result, key, source, target, shards_of, factor):
    owner, partner = [(jnp.arange(result.shape[axis_at]) // (result.shape[axis_at] // shards_of)).reshape([-1 if axis == axis_at else 1 for axis in range(result.ndim)]) for axis_at in (source, target)]
    chosen = jax.random.permutation(key, shards_of)[partner]
    strong = (owner == chosen) | (owner == (partner + shards_of // 2) % shards_of)
    return jnp.where(strong, factor * result, result)


def block_levels(own_key, shape, shards, smallest, high):
    loudness = 1.0
    for axis_at, parts in shards:
        heights = jax.random.uniform(jax.random.fold_in(jax.random.fold_in(own_key, 6), axis_at), (parts,), jnp.float32, smallest / len(shards), high / len(shards))
        loudness = loudness * jnp.repeat(jnp.exp(heights), shape[axis_at] // parts).reshape((-1,) + (1,) * (len(shape) - 1 - axis_at))
    return loudness


def gaussian(own_key, shape, scale, most, cuts=(), kind=jnp.bfloat16):
    values = scale * jax.random.normal(own_key, shape, jnp.float32)
    if cuts:
        values = values * block_levels(own_key, shape, cuts, -0.22, 0.18)
    return jnp.clip(values, -most, most).astype(kind)


def gaussian_with(own_key, dims, deviation, reach, shards, heavy, kind=jnp.bfloat16):
    values = deviation * jax.random.normal(own_key, dims, jnp.float32)
    if shards:
        values = values * block_levels(own_key, dims, shards, -0.22, 0.18)
    return jnp.clip(raised(values, jax.random.fold_in(own_key, 3), *heavy), -reach, reach).astype(kind)


def setup_inputs(seed: int = 0) -> dict:
    key_of = jax.random.split(jax.random.key(seed), 12)
    saved_inputs = gaussian_with(key_of[0], (TOKENS, D), 1.0, 8.0, ((0, 16),), (0, 1, 16, 2.0))
    input_cot = gaussian(key_of[1], (TOKENS, W), (TOKENS ** -0.5), 0.0546875, ((0, 16), (1, 2)))
    gate_cot = gaussian(key_of[2], (TOKENS, W), (TOKENS ** -0.5), 0.0546875, ((0, 16), (1, 2)))
    input_master = gaussian(key_of[3], (D, W), 1.0, 6.0, ((0, 16), (1, 2)), jnp.float32)
    gate_master = gaussian(key_of[4], (D, W), 1.0, 6.0, ((0, 16), (1, 2)), jnp.float32)
    input_factor = draw_input_factor(jax.random.fold_in(key_of[11], 71), 0)
    gate_factor = draw_gate_factor(jax.random.fold_in(key_of[11], 71), 0)
    input_first = gaussian(key_of[7], (RANK, W), 1.0, 6.0, ((0, 16), (1, 2)), jnp.float32)
    input_second = draw_input_second(jax.random.fold_in(key_of[11], 71), 0)
    gate_first = gaussian(key_of[9], (RANK, W), 1.0, 6.0, ((0, 16), (1, 2)), jnp.float32)
    gate_second = draw_gate_second(jax.random.fold_in(key_of[11], 71), 0)
    return {"saved_inputs": saved_inputs, "input_cot": input_cot, "gate_cot": gate_cot, "input_master": input_master, "gate_master": gate_master, "input_factor": input_factor, "gate_factor": gate_factor, "input_first": input_first, "input_second": input_second, "gate_first": gate_first, "gate_second": gate_second}


first_decay = 0.9
second_decay = 0.9
ratio_floor = 1e-08
mean_floor = 1e-06
step_size = 0.05

def update_one(saved_inputs, cotangent, master, factor, first, second):
    contract = (((0,), (0,)), ((), ()))
    gradient = lax.dot_general(saved_inputs, cotangent, contract, preferred_element_type=jnp.float32)
    factor_wide = factor.astype(jnp.float32)
    low_rank = lax.dot_general(factor_wide, gradient, contract, precision=lax.Precision.HIGHEST)
    first_new = first_decay * first + (1.0 - first_decay) * low_rank
    second_new = second_decay * second + (1.0 - second_decay) * low_rank * low_rank
    ratio = first_new / (jnp.sqrt(second_new) + ratio_floor)
    direction = jnp.dot(factor_wide, ratio, precision=lax.Precision.HIGHEST)
    step = direction * lax.rsqrt(jnp.mean(direction * direction) + mean_floor)
    weights_copy = (master - step_size * step).astype(jnp.bfloat16)
    return (step, first_new, second_new, weights_copy)

def reference(saved_inputs, input_cot, gate_cot, input_master, gate_master, input_factor, gate_factor, input_first, input_second, gate_first, gate_second):
    step_in, first_in, second_in, copy_in = update_one(saved_inputs, input_cot, input_master, input_factor, input_first, input_second)
    step_gate, first_gate, second_gate, copy_gate = update_one(saved_inputs, gate_cot, gate_master, gate_factor, gate_first, gate_second)
    return (step_in, step_gate, first_in, second_in, first_gate, second_gate, copy_in, copy_gate)
```

```python
import functools

import jax
import jax.numpy as jnp
from jax import lax
from jax.experimental import pallas as pl
from jax.experimental.pallas import tpu as pltpu
from jax.sharding import PartitionSpec as P

first_decay = 0.9
second_decay = 0.9
ratio_floor = 1e-08
mean_floor = 1e-06
step_size = 0.05
PLANE = 4
VMEM = pltpu.VMEM
DMA = pltpu.SemaphoreType.DMA
MESH = pl.DeviceIdType.MESH


class Place:
    def __init__(self, n):
        self.n = n
        self.depth = n // PLANE
        self.f = lax.axis_index("fs")
        self.z = lax.div(self.f, PLANE)
        self.spot = lax.rem(self.f, PLANE)
        self.x = lax.rem(self.f, 2)
        self.y = lax.div(self.spot, 2)
        self.fx = self.f + 1 - 2 * self.x
        self.fy = self.f + 2 - 4 * self.y
        self.sx = self.spot + 1 - 2 * self.x
        self.sy = self.spot + 2 - 4 * self.y

    def plane(self, dz):
        return lax.rem(self.z + dz + self.depth, self.depth)


def send(src, dst, s_sem, r_sem, axis, target):
    return pltpu.make_async_remote_copy(
        src_ref=src,
        dst_ref=dst,
        send_sem=s_sem,
        recv_sem=r_sem,
        device_id={axis: target},
        device_id_type=MESH,
    )


def greet(targets):
    barrier = pltpu.get_barrier_semaphore()
    for axis, target in targets:
        pl.semaphore_signal(barrier, inc=1, device_id={axis: target}, device_id_type=MESH)
    pl.semaphore_wait(barrier, len(targets))


def gather(at, a, b, s_z, r_z, s_p, r_p):
    depth = at.depth
    started = []

    def go(copy):
        copy.start()
        started.append(copy)
        return copy

    far = [None]
    for dz in range(1, depth):
        target = at.plane(dz) * PLANE + at.spot
        far.append(
            (
                go(send(a.at[at.f], a.at[at.f], s_z.at[dz, 0], r_z.at[dz, 0], "fs", target)),
                go(send(b.at[at.f], b.at[at.f], s_z.at[dz, 1], r_z.at[dz, 1], "fs", target)),
            )
        )
    near = []
    for s in range(depth + 1):
        if s < depth:
            base = at.plane(-s) * PLANE
            mine = base + at.spot

            def own(ref, k, target):
                return go(send(ref.at[mine], ref.at[mine], s_p.at[s, k], r_p.at[s, k], "fs", target))

            if s > 0:
                far[s][0].wait_recv()
            xa = own(a, 0, at.fx)
            ya = own(a, 1, at.fy)
            if s > 0:
                far[s][1].wait_recv()
            yb = own(b, 2, at.fy)
            xb = own(b, 3, at.fx)
            near.append((base, xa, ya, yb, xb))
        if s > 0:
            base, xa, ya, yb, xb = near[s - 1]
            xa.wait_recv()
            got = base + at.sx
            ra = go(send(a.at[got], a.at[got], s_p.at[s - 1, 4], r_p.at[s - 1, 4], "fs", at.fy))
            yb.wait_recv()
            got = base + at.sy
            rb = go(send(b.at[got], b.at[got], s_p.at[s - 1, 5], r_p.at[s - 1, 5], "fs", at.fx))
            near[s - 1] = (ya, xb, ra, rb)
    for group in near:
        for copy in group:
            copy.wait_recv()
    for copy in started:
        copy.wait_send()


def near_targets(at):
    return [("fs", at.fx), ("fs", at.fy)] + [
        ("fs", at.plane(dz) * PLANE + at.spot) for dz in range(1, at.depth)
    ]


def factor_kernel(n, a_ref, b_ref, a_out, b_out, s_z, r_z, s_p, r_p):
    at = Place(n)
    a_out[at.f] = a_ref[...]
    b_out[at.f] = b_ref[...]
    greet(near_targets(at))
    gather(at, a_out, b_out, s_z, r_z, s_p, r_p)


def gather_sems(n):
    depth = n // PLANE
    return [DMA((depth, 2)), DMA((depth, 2)), DMA((depth, 6)), DMA((depth, 6))]


def moments(low_rank, first, second):
    first_new = first_decay * first + (1.0 - first_decay) * low_rank
    second_new = second_decay * second + (1.0 - second_decay) * low_rank * low_rank
    ratio = first_new / (jnp.sqrt(second_new) + ratio_floor)
    return (first_new, second_new, ratio)


def wide_dot(narrow, wide):
    total = None
    rest = wide
    for _ in range(3):
        part = rest.astype(jnp.bfloat16)
        rest = rest - part.astype(jnp.float32)
        term = jnp.dot(narrow, part, preferred_element_type=jnp.float32)
        total = term if total is None else total + term
    return total


def main_kernel(
    n,
    m,
    term_a,
    term_b,
    first_a,
    second_a,
    first_b,
    second_b,
    factor_a,
    factor_b,
    master_a,
    master_b,
    step_a,
    step_b,
    first_a_new,
    second_a_new,
    first_b_new,
    second_b_new,
    copy_a,
    copy_b,
    one_a,
    one_b,
    two_a,
    two_b,
    sum_a,
    sum_b,
    ready_a,
    ready_b,
    far_a,
    far_b,
    all_a,
    all_b,
    pair,
    total,
    s_one,
    r_one,
    s_two,
    r_two,
    s_far,
    r_far,
    rz_s,
    rz_r,
    rp_s,
    rp_r,
    s_tp,
    r_tp,
    s_fs,
    r_fs,
    cz_s,
    cz_r,
    cp_s,
    cp_r,
):
    at = Place(n)
    depth = at.depth
    t = lax.axis_index("tp")
    others = [lax.rem(at.f + k, n) for k in range(1, n)]
    mates = [lax.rem(t + k, m) for k in range(1, m)]
    greet([("fs", o) for o in others] + [("tp", o) for o in mates])
    started = []

    def go(copy):
        copy.start()
        started.append(copy)
        return copy

    first_stage = []
    for k in range(depth):
        plane = at.plane(k + 1)
        pair_a = go(send(term_a.at[plane, :, 1 - at.x], one_a.at[k], s_one.at[k, 0], r_one.at[k, 0], "fs", at.fx))
        pair_b = go(send(term_b.at[plane, 1 - at.y], one_b.at[k], s_one.at[k, 1], r_one.at[k, 1], "fs", at.fy))
        first_stage.append((pair_a, pair_b))
    second_stage = []
    third_stage = []
    for k in range(depth + 1):
        if k < depth:
            plane = at.plane(k + 1)
            first_stage[k][0].wait_recv()
            sum_a[k] = term_a[plane, :, at.x] + one_a[k]
            ca = go(send(sum_a.at[k, 1 - at.y], two_a.at[k], s_two.at[k, 0], r_two.at[k, 0], "fs", at.fy))
            first_stage[k][1].wait_recv()
            sum_b[k] = term_b[plane, at.y] + one_b[k]
            cb = go(send(sum_b.at[k, 1 - at.x], two_b.at[k], s_two.at[k, 1], r_two.at[k, 1], "fs", at.fx))
            second_stage.append((ca, cb))
        if k > 0:
            j = k - 1
            target = at.plane(k) * PLANE + at.spot
            second_stage[j][0].wait_recv()
            ready_a[j] = sum_a[j, at.y] + two_a[j]
            if j < depth - 1:
                ca = go(send(ready_a.at[j], far_a.at[j], s_far.at[j, 0], r_far.at[j, 0], "fs", target))
            second_stage[j][1].wait_recv()
            ready_b[j] = sum_b[j, at.x] + two_b[j]
            if j < depth - 1:
                cb = go(send(ready_b.at[j], far_b.at[j], s_far.at[j, 1], r_far.at[j, 1], "fs", target))
                third_stage.append((ca, cb))
    low_a = ready_a[depth - 1]
    low_b = ready_b[depth - 1]
    for j in range(depth - 1):
        third_stage[j][0].wait_recv()
        low_a = low_a + far_a[j]
        third_stage[j][1].wait_recv()
        low_b = low_b + far_b[j]

    new_first, new_second, ratio = moments(low_a, first_a[...], second_a[...])
    first_a_new[...] = new_first
    second_a_new[...] = new_second
    all_a[at.f] = ratio
    new_first, new_second, ratio = moments(low_b, first_b[...], second_b[...])
    first_b_new[...] = new_first
    second_b_new[...] = new_second
    all_b[at.f] = ratio

    gather(at, all_a, all_b, rz_s, rz_r, rp_s, rp_r)

    rank = all_a.shape[0] * all_a.shape[1]
    cols = all_a.shape[2]
    dir_a = wide_dot(factor_a[...], all_a[...].reshape(rank, cols))
    dir_b = wide_dot(factor_b[...], all_b[...].reshape(rank, cols))
    count = n * dir_a.shape[0] * m * cols

    pair[0, 0:8] = jnp.full((8, 128), jnp.sum(dir_a * dir_a), jnp.float32)
    pair[0, 8:16] = jnp.full((8, 128), jnp.sum(dir_b * dir_b), jnp.float32)
    trips = [
        go(send(pair.at[0], pair.at[k + 1], s_tp.at[k], r_tp.at[k], "tp", mate)) for k, mate in enumerate(mates)
    ]
    step_a[...] = dir_a
    step_b[...] = dir_b
    joint = pair[0]
    for k, trip in enumerate(trips):
        trip.wait_recv()
        joint = joint + pair[k + 1]
    total[0] = joint
    trips = [
        go(send(total.at[0], total.at[k + 1], s_fs.at[k], r_fs.at[k], "fs", other)) for k, other in enumerate(others)
    ]
    joint = total[0]
    for k, trip in enumerate(trips):
        trip.wait_recv()
        joint = joint + total[k + 1]
    scale = lax.rsqrt(joint / count + mean_floor)
    new_step = step_a[...] * scale[0:1, 0:1]
    step_a[...] = new_step
    copy_a[at.f] = (master_a[...] - step_size * new_step).astype(jnp.bfloat16)
    new_step = step_b[...] * scale[8:9, 0:1]
    step_b[...] = new_step
    copy_b[at.f] = (master_b[...] - step_size * new_step).astype(jnp.bfloat16)

    gather(at, copy_a, copy_b, cz_s, cz_r, cp_s, cp_r)
    for copy in started:
        copy.wait_send()


def local(
    n,
    m,
    saved_inputs,
    input_cot,
    gate_cot,
    input_master,
    gate_master,
    input_factor,
    gate_factor,
    input_first,
    input_second,
    gate_first,
    gate_second,
):
    in_vmem = pl.BlockSpec(memory_space=VMEM)
    rows, rank = input_factor.shape
    low_rows, cols = input_first.shape
    depth = n // PLANE
    shape = jax.ShapeDtypeStruct
    f32, bf16 = jnp.float32, jnp.bfloat16
    whole_in, whole_gate = pl.pallas_call(
        functools.partial(factor_kernel, n),
        out_shape=[shape((n, rows, rank), bf16)] * 2,
        in_specs=[in_vmem] * 2,
        out_specs=[in_vmem] * 2,
        scratch_shapes=gather_sems(n),
        compiler_params=pltpu.CompilerParams(collective_id=0, has_side_effects=True),
        name="factors",
    )(input_factor, gate_factor)

    def term(whole, cot):
        mid = jnp.dot(saved_inputs, whole.reshape(n * rows, rank), preferred_element_type=f32)
        low = lax.dot_general(
            mid, cot.astype(f32), (((0,), (0,)), ((), ())), precision=lax.Precision.HIGHEST
        )
        return low.reshape(depth, 2, 2, low_rows, cols)

    term_in = term(whole_in, input_cot)
    term_gate = term(whole_gate, gate_cot)
    low = shape((low_rows, cols), f32)
    piece = (low_rows, cols)
    full = shape((rows, cols), f32)
    copies = shape((n, rows, cols), bf16)
    outs = pl.pallas_call(
        functools.partial(main_kernel, n, m),
        out_shape=[full, full, low, low, low, low, copies, copies],
        in_specs=[in_vmem] * 10,
        out_specs=[in_vmem] * 8,
        scratch_shapes=[
            VMEM((depth, 2) + piece, f32),
            VMEM((depth, 2) + piece, f32),
            VMEM((depth,) + piece, f32),
            VMEM((depth,) + piece, f32),
            VMEM((depth, 2) + piece, f32),
            VMEM((depth, 2) + piece, f32),
            VMEM((depth,) + piece, f32),
            VMEM((depth,) + piece, f32),
            VMEM((depth,) + piece, f32),
            VMEM((depth,) + piece, f32),
            VMEM((n,) + piece, f32),
            VMEM((n,) + piece, f32),
            VMEM((m, 16, 128), f32),
            VMEM((n, 16, 128), f32),
            DMA((depth, 2)),
            DMA((depth, 2)),
            DMA((depth, 2)),
            DMA((depth, 2)),
            DMA((depth, 2)),
            DMA((depth, 2)),
            *gather_sems(n),
            DMA((m,)),
            DMA((m,)),
            DMA((n,)),
            DMA((n,)),
            *gather_sems(n),
        ],
        compiler_params=pltpu.CompilerParams(
            collective_id=1, has_side_effects=True, vmem_limit_bytes=56 * 2**20
        ),
        name="update",
    )(
        term_in,
        term_gate,
        input_first,
        input_second,
        gate_first,
        gate_second,
        input_factor,
        gate_factor,
        input_master,
        gate_master,
    )
    *head, copy_in, copy_gate = outs
    return (*head, copy_in.reshape(n * rows, cols), copy_gate.reshape(n * rows, cols))


def solution(mesh):
    n, m = mesh.shape["fs"], mesh.shape["tp"]
    both = P("fs", "tp")
    rows = P("fs", None)
    return jax.shard_map(
        functools.partial(local, n, m),
        mesh=mesh,
        in_specs=(rows, both, both, both, both, rows, rows, both, both, both, both),
        out_specs=(both,) * 6 + (P(None, "tp"),) * 2,
        check_vma=False,
    )
```

```python
import functools

import jax
import jax.numpy as jnp
from jax import lax
from jax.experimental import pallas as pl
from jax.experimental.pallas import tpu as pltpu
from jax.sharding import PartitionSpec as P

first_decay = 0.9
second_decay = 0.9
ratio_floor = 1e-08
mean_floor = 1e-06
step_size = 0.05
PLANE = 4
VMEM = pltpu.VMEM
DMA = pltpu.SemaphoreType.DMA
MESH = pl.DeviceIdType.MESH


class Place:
    def __init__(self, n):
        self.n = n
        self.depth = n // PLANE
        self.f = lax.axis_index("fs")
        self.z = lax.div(self.f, PLANE)
        self.spot = lax.rem(self.f, PLANE)
        self.x = lax.rem(self.f, 2)
        self.y = lax.div(self.spot, 2)
        self.fx = self.f + 1 - 2 * self.x
        self.fy = self.f + 2 - 4 * self.y
        self.sx = self.spot + 1 - 2 * self.x
        self.sy = self.spot + 2 - 4 * self.y

    def twin(self, s):
        other = self.z
        bit = 1
        while bit <= s:
            if s // bit % 2:
                other = other + bit - 2 * bit * lax.rem(lax.div(self.z, bit), 2)
            bit *= 2
        return other


def send(src, dst, s_sem, r_sem, axis, target):
    return pltpu.make_async_remote_copy(
        src_ref=src,
        dst_ref=dst,
        send_sem=s_sem,
        recv_sem=r_sem,
        device_id={axis: target},
        device_id_type=MESH,
    )


def greet(targets):
    barrier = pltpu.get_barrier_semaphore()
    for axis, target in targets:
        pl.semaphore_signal(barrier, inc=1, device_id={axis: target}, device_id_type=MESH)
    pl.semaphore_wait(barrier, len(targets))


def whole_block(ref, index):
    return ref.at[index]


def gather(at, a, b, s_z, r_z, s_p, r_p, view=whole_block, arrived=None):
    depth = at.depth
    started = []

    def go(ref, index, s_sem, r_sem, target):
        copy = send(view(ref, index), view(ref, index), s_sem, r_sem, "fs", target)
        copy.start()
        started.append(copy)
        return copy

    far = [None]

    def reach(dz):
        target = at.twin(dz) * PLANE + at.spot
        far.append(
            (
                go(a, at.f, s_z.at[dz, 0], r_z.at[dz, 0], target),
                go(b, at.f, s_z.at[dz, 1], r_z.at[dz, 1], target),
            )
        )

    near = []
    for s in range(depth):
        base = at.twin(s) * PLANE
        mine = base + at.spot
        if s > 0:
            far[s][0].wait_recv()
        xa = go(a, mine, s_p.at[s, 0], r_p.at[s, 0], at.fx)
        ya = go(a, mine, s_p.at[s, 1], r_p.at[s, 1], at.fy)
        if s > 0:
            far[s][1].wait_recv()
        yb = go(b, mine, s_p.at[s, 2], r_p.at[s, 2], at.fy)
        xb = go(b, mine, s_p.at[s, 3], r_p.at[s, 3], at.fx)
        if s == 0:
            for dz in range(1, depth):
                reach(dz)
        xa.wait_recv()
        ra = go(a, base + at.sx, s_p.at[s, 4], r_p.at[s, 4], at.fy)
        yb.wait_recv()
        rb = go(b, base + at.sy, s_p.at[s, 5], r_p.at[s, 5], at.fx)
        near.append((base, ya, xb, ra, rb))
    for base, *group in near:
        for copy in group:
            copy.wait_recv()
        if arrived is not None:
            arrived(base)
    for copy in started:
        copy.wait_send()


def gather_sems(n):
    depth = n // PLANE
    return [DMA((depth, 2)), DMA((depth, 2)), DMA((depth, 6)), DMA((depth, 6))]


def moments(low_rank, first, second):
    first_new = first_decay * first + (1.0 - first_decay) * low_rank
    second_new = second_decay * second + (1.0 - second_decay) * low_rank * low_rank
    ratio = first_new / (jnp.sqrt(second_new) + ratio_floor)
    return (first_new, second_new, ratio)


def wide_dot(narrow, wide):
    total = None
    rest = wide
    for _ in range(3):
        part = rest.astype(jnp.bfloat16)
        rest = rest - part.astype(jnp.float32)
        term = jnp.dot(narrow, part, preferred_element_type=jnp.float32)
        total = term if total is None else total + term
    return total


def main_kernel(
    n,
    m,
    saved_hbm,
    cot_a_hbm,
    cot_b_hbm,
    master_a_hbm,
    master_b_hbm,
    factor_a,
    factor_b,
    first_a,
    second_a,
    first_b,
    second_b,
    step_a,
    step_b,
    first_a_new,
    second_a_new,
    first_b_new,
    second_b_new,
    copy_a_hbm,
    copy_b_hbm,
    saved,
    cot_a,
    cot_b,
    master_a,
    master_b,
    whole_a,
    whole_b,
    mid_a,
    mid_b,
    term_a,
    term_b,
    copy_a,
    copy_b,
    one_a,
    one_b,
    two_a,
    two_b,
    sum_a,
    sum_b,
    ready_a,
    ready_b,
    far_a,
    far_b,
    all_a,
    all_b,
    pair,
    total,
    load_sem,
    store_sem,
    s_mate,
    r_mate,
    s_one,
    r_one,
    s_two,
    r_two,
    s_far,
    r_far,
    fz_s,
    fz_r,
    fp_s,
    fp_r,
    rz_s,
    rz_r,
    rp_s,
    rp_r,
    s_tp,
    r_tp,
    s_fs,
    r_fs,
    cz_s,
    cz_r,
    cp_s,
    cp_r,
):
    at = Place(n)
    depth = at.depth
    t = lax.axis_index("tp")
    others = [lax.rem(at.f + k, n) for k in range(1, n)]
    mates = [lax.rem(t + k, m) for k in range(1, m)]
    loads = [
        pltpu.make_async_copy(src, dst, load_sem.at[k])
        for k, (src, dst) in enumerate(
            (
                (saved_hbm, saved),
                (cot_a_hbm, cot_a),
                (cot_b_hbm, cot_b),
                (master_a_hbm, master_a),
                (master_b_hbm, master_b),
            )
        )
    ]
    for load in loads:
        load.start()
    whole_a[at.f] = factor_a[...]
    whole_b[at.f] = factor_b[...]
    greet([("fs", o) for o in others] + [("tp", o) for o in mates])
    started = []

    def go(copy):
        copy.start()
        started.append(copy)
        return copy

    rows = factor_a.shape[0]
    parts = 2 if m % 2 == 0 else 1
    mate = t + 1 - 2 * lax.rem(t, 2)
    half = pl.ds(pl.multiple_of(lax.rem(t, 2) * (rows // 2), rows // 2), rows // 2) if parts == 2 else pl.ds(0, rows)
    passed = []
    width = PLANE * rows

    def multiply(k):
        base, copies = passed[k]
        for copy in copies:
            copy.wait_recv()
        if k == 0:
            loads[0].wait()
        columns = pl.ds(pl.multiple_of(base * rows, width), width)
        for mid, whole in ((mid_a, whole_a), (mid_b, whole_b)):
            block = whole[pl.ds(base, PLANE)].reshape(width, whole.shape[2])
            product = jnp.dot(saved[:, columns], block, preferred_element_type=jnp.float32)
            if k == 0:
                mid[...] = product
            else:
                mid[...] += product

    def arrived(base):
        k = len(passed)
        copies = []
        if parts == 2:
            for side, whole in enumerate((whole_a, whole_b)):
                view = whole.at[pl.ds(base, PLANE), half]
                copies.append(go(send(view, view, s_mate.at[k, side], r_mate.at[k, side], "tp", mate)))
        passed.append((base, copies))
        if k > 0:
            multiply(k - 1)

    gather(at, whole_a, whole_b, fz_s, fz_r, fp_s, fp_r, lambda ref, index: ref.at[index, half], arrived)
    multiply(depth - 1)

    def project(mid, cot):
        rest = mid[...].T
        result = None
        for _ in range(3):
            part = rest.astype(jnp.bfloat16)
            rest = rest - part.astype(jnp.float32)
            piece = jnp.dot(part, cot[...], preferred_element_type=jnp.float32)
            result = piece if result is None else result + piece
        return result

    loads[1].wait()
    term_a[...] = project(mid_a, cot_a).reshape(term_a.shape)
    first_a_stage = []
    for k in range(depth):
        plane = at.twin(depth - 1 - k)
        first_a_stage.append(
            go(send(term_a.at[plane, :, 1 - at.x], one_a.at[k], s_one.at[k, 0], r_one.at[k, 0], "fs", at.fx))
        )
    loads[2].wait()
    term_b[...] = project(mid_b, cot_b).reshape(term_b.shape)
    first_stage = []
    for k in range(depth):
        plane = at.twin(depth - 1 - k)
        pair_b = go(send(term_b.at[plane, 1 - at.y], one_b.at[k], s_one.at[k, 1], r_one.at[k, 1], "fs", at.fy))
        first_stage.append((first_a_stage[k], pair_b))
    second_stage = []
    third_stage = []
    for k in range(depth + 1):
        if k < depth:
            plane = at.twin(depth - 1 - k)
            first_stage[k][0].wait_recv()
            sum_a[k] = term_a[plane, :, at.x] + one_a[k]
            ca = go(send(sum_a.at[k, 1 - at.y], two_a.at[k], s_two.at[k, 0], r_two.at[k, 0], "fs", at.fy))
            first_stage[k][1].wait_recv()
            sum_b[k] = term_b[plane, at.y] + one_b[k]
            cb = go(send(sum_b.at[k, 1 - at.x], two_b.at[k], s_two.at[k, 1], r_two.at[k, 1], "fs", at.fx))
            second_stage.append((ca, cb))
        if k > 0:
            j = k - 1
            target = at.twin(depth - k) * PLANE + at.spot
            second_stage[j][0].wait_recv()
            ready_a[j] = sum_a[j, at.y] + two_a[j]
            if j < depth - 1:
                ca = go(send(ready_a.at[j], far_a.at[j], s_far.at[j, 0], r_far.at[j, 0], "fs", target))
            second_stage[j][1].wait_recv()
            ready_b[j] = sum_b[j, at.x] + two_b[j]
            if j < depth - 1:
                cb = go(send(ready_b.at[j], far_b.at[j], s_far.at[j, 1], r_far.at[j, 1], "fs", target))
                third_stage.append((ca, cb))
    low_a = ready_a[depth - 1]
    low_b = ready_b[depth - 1]
    for j in range(depth - 1):
        third_stage[j][0].wait_recv()
        low_a = low_a + far_a[j]
        third_stage[j][1].wait_recv()
        low_b = low_b + far_b[j]

    new_first, new_second, ratio = moments(low_a, first_a[...], second_a[...])
    first_a_new[...] = new_first
    second_a_new[...] = new_second
    all_a[at.f] = ratio
    new_first, new_second, ratio = moments(low_b, first_b[...], second_b[...])
    first_b_new[...] = new_first
    second_b_new[...] = new_second
    all_b[at.f] = ratio

    gather(at, all_a, all_b, rz_s, rz_r, rp_s, rp_r)

    rank = all_a.shape[0] * all_a.shape[1]
    cols = all_a.shape[2]
    dir_a = wide_dot(factor_a[...], all_a[...].reshape(rank, cols))
    dir_b = wide_dot(factor_b[...], all_b[...].reshape(rank, cols))
    count = n * dir_a.shape[0] * m * cols

    pair[0, 0:8] = jnp.full((8, 128), jnp.sum(dir_a * dir_a), jnp.float32)
    pair[0, 8:16] = jnp.full((8, 128), jnp.sum(dir_b * dir_b), jnp.float32)
    trips = [
        go(send(pair.at[0], pair.at[k + 1], s_tp.at[k], r_tp.at[k], "tp", mate)) for k, mate in enumerate(mates)
    ]
    step_a[...] = dir_a
    step_b[...] = dir_b
    joint = pair[0]
    for k, trip in enumerate(trips):
        trip.wait_recv()
        joint = joint + pair[k + 1]
    total[0] = joint
    trips = [
        go(send(total.at[0], total.at[k + 1], s_fs.at[k], r_fs.at[k], "fs", other)) for k, other in enumerate(others)
    ]
    joint = total[0]
    for k, trip in enumerate(trips):
        trip.wait_recv()
        joint = joint + total[k + 1]
    scale = lax.rsqrt(joint / count + mean_floor)
    new_step = step_a[...] * scale[0:1, 0:1]
    step_a[...] = new_step
    loads[3].wait()
    copy_a[at.f] = (master_a[...] - step_size * new_step).astype(jnp.bfloat16)
    new_step = step_b[...] * scale[8:9, 0:1]
    step_b[...] = new_step
    loads[4].wait()
    copy_b[at.f] = (master_b[...] - step_size * new_step).astype(jnp.bfloat16)

    stores = []

    def put(base):
        k = len(stores)
        block = pl.ds(base, PLANE)
        for side, (src, dst) in enumerate(((copy_a, copy_a_hbm), (copy_b, copy_b_hbm))):
            stores.append(pltpu.make_async_copy(src.at[block], dst.at[block], store_sem.at[k + side]))
            stores[-1].start()

    gather(at, copy_a, copy_b, cz_s, cz_r, cp_s, cp_r, whole_block, put)
    for store in stores:
        store.wait()
    for copy in started:
        copy.wait_send()


def hand_kernel(depth, *refs):
    count = (len(refs) - 2) // 3
    given, out, held = refs[:count], refs[count : 2 * count], refs[2 * count : 3 * count]
    in_sem, out_sem = refs[3 * count :]
    moves = []
    for k in range(count):
        pieces = depth if len(given[k].shape) == 3 else 1
        size = given[k].shape[0] // pieces
        for i in range(pieces):
            part = pl.ds(i * size, size)
            moves.append(
                (
                    pltpu.make_async_copy(given[k].at[part], held[k].at[part], in_sem.at[k, i]),
                    pltpu.make_async_copy(held[k].at[part], out[k].at[part], out_sem.at[k, i]),
                )
            )
    for into, _ in moves:
        into.start()
    for into, onward in moves:
        into.wait()
        onward.start()
    for _, onward in moves:
        onward.wait()


def local(
    n,
    m,
    saved_inputs,
    input_cot,
    gate_cot,
    input_master,
    gate_master,
    input_factor,
    gate_factor,
    input_first,
    input_second,
    gate_first,
    gate_second,
):
    in_vmem = pl.BlockSpec(memory_space=VMEM)
    anywhere = pl.BlockSpec(memory_space=pl.ANY)
    rows, rank = input_factor.shape
    tokens = saved_inputs.shape[0]
    low_rows, cols = input_first.shape
    depth = n // PLANE
    shape = jax.ShapeDtypeStruct
    f32, bf16 = jnp.float32, jnp.bfloat16
    low = shape((low_rows, cols), f32)
    piece = (low_rows, cols)
    full = shape((rows, cols), f32)
    copies = shape((n, rows, cols), bf16)
    shapes = [full, full, low, low, low, low, copies, copies]
    outs = pl.pallas_call(
        functools.partial(main_kernel, n, m),
        out_shape=shapes,
        in_specs=[anywhere] * 5 + [in_vmem] * 6,
        out_specs=[in_vmem] * 6 + [anywhere] * 2,
        scratch_shapes=[
            VMEM(saved_inputs.shape, bf16),
            VMEM(input_cot.shape, bf16),
            VMEM(input_cot.shape, bf16),
            VMEM((rows, cols), f32),
            VMEM((rows, cols), f32),
            VMEM((n, rows, rank), bf16),
            VMEM((n, rows, rank), bf16),
            VMEM((tokens, rank), f32),
            VMEM((tokens, rank), f32),
            VMEM((depth, 2, 2) + piece, f32),
            VMEM((depth, 2, 2) + piece, f32),
            VMEM((n, rows, cols), bf16),
            VMEM((n, rows, cols), bf16),
            VMEM((depth, 2) + piece, f32),
            VMEM((depth, 2) + piece, f32),
            VMEM((depth,) + piece, f32),
            VMEM((depth,) + piece, f32),
            VMEM((depth, 2) + piece, f32),
            VMEM((depth, 2) + piece, f32),
            VMEM((depth,) + piece, f32),
            VMEM((depth,) + piece, f32),
            VMEM((depth,) + piece, f32),
            VMEM((depth,) + piece, f32),
            VMEM((n,) + piece, f32),
            VMEM((n,) + piece, f32),
            VMEM((m, 16, 128), f32),
            VMEM((n, 16, 128), f32),
            DMA((5,)),
            DMA((2 * depth,)),
            *[DMA((depth, 2))] * 8,
            *gather_sems(n),
            *gather_sems(n),
            DMA((m,)),
            DMA((m,)),
            DMA((n,)),
            DMA((n,)),
            *gather_sems(n),
        ],
        compiler_params=pltpu.CompilerParams(
            collective_id=1, has_side_effects=True, vmem_limit_bytes=56 * 2**20
        ),
        name="update",
    )(
        saved_inputs,
        input_cot,
        gate_cot,
        input_master,
        gate_master,
        input_factor,
        gate_factor,
        input_first,
        input_second,
        gate_first,
        gate_second,
    )
    outs = pl.pallas_call(
        functools.partial(hand_kernel, depth),
        out_shape=shapes,
        in_specs=[anywhere] * 8,
        out_specs=[anywhere] * 8,
        scratch_shapes=[VMEM(s.shape, s.dtype) for s in shapes] + [DMA((8, depth))] * 2,
        name="results",
    )(*outs)
    *head, copy_in, copy_gate = outs
    return (*head, copy_in.reshape(n * rows, cols), copy_gate.reshape(n * rows, cols))


def solution(mesh):
    n, m = mesh.shape["fs"], mesh.shape["tp"]
    both = P("fs", "tp")
    rows = P("fs", None)
    return jax.shard_map(
        functools.partial(local, n, m),
        mesh=mesh,
        in_specs=(rows, both, both, both, both, rows, rows, both, both, both, both),
        out_specs=(both,) * 6 + (P(None, "tp"),) * 2,
        check_vma=False,
    )
```

```python
import functools

import jax
import jax.numpy as jnp
from jax import lax
from jax.experimental import pallas as pl
from jax.experimental.pallas import tpu as pltpu
from jax.sharding import PartitionSpec as P

first_decay = 0.9
second_decay = 0.9
ratio_floor = 1e-08
mean_floor = 1e-06
step_size = 0.05
PLANE = 4
VMEM = pltpu.VMEM
DMA = pltpu.SemaphoreType.DMA
MESH = pl.DeviceIdType.MESH


class Place:
    def __init__(self, n):
        self.n = n
        self.depth = n // PLANE
        self.f = lax.axis_index("fs")
        self.z = lax.div(self.f, PLANE)
        self.spot = lax.rem(self.f, PLANE)
        self.x = lax.rem(self.f, 2)
        self.y = lax.div(self.spot, 2)
        self.fx = self.f + 1 - 2 * self.x
        self.fy = self.f + 2 - 4 * self.y
        self.sx = self.spot + 1 - 2 * self.x
        self.sy = self.spot + 2 - 4 * self.y

    def twin(self, s):
        other = self.z
        bit = 1
        while bit <= s:
            if s // bit % 2:
                other = other + bit - 2 * bit * lax.rem(lax.div(self.z, bit), 2)
            bit *= 2
        return other


def send(src, dst, s_sem, r_sem, axis, target):
    return pltpu.make_async_remote_copy(
        src_ref=src,
        dst_ref=dst,
        send_sem=s_sem,
        recv_sem=r_sem,
        device_id={axis: target},
        device_id_type=MESH,
    )


def greet(targets):
    barrier = pltpu.get_barrier_semaphore()
    for axis, target in targets:
        pl.semaphore_signal(barrier, inc=1, device_id={axis: target}, device_id_type=MESH)
    pl.semaphore_wait(barrier, len(targets))


def whole_block(ref, index):
    return ref.at[index]


def gather(at, a, b, s_z, r_z, s_p, r_p, view=whole_block, arrived=None):
    depth = at.depth
    started = []

    def go(ref, index, s_sem, r_sem, target):
        copy = send(view(ref, index), view(ref, index), s_sem, r_sem, "fs", target)
        copy.start()
        started.append(copy)
        return copy

    far = [None]

    def reach(dz):
        target = at.twin(dz) * PLANE + at.spot
        far.append(
            (
                go(a, at.f, s_z.at[dz, 0], r_z.at[dz, 0], target),
                go(b, at.f, s_z.at[dz, 1], r_z.at[dz, 1], target),
            )
        )

    near = []
    for s in range(depth):
        base = at.twin(s) * PLANE
        mine = base + at.spot
        if s > 0:
            far[s][0].wait_recv()
        xa = go(a, mine, s_p.at[s, 0], r_p.at[s, 0], at.fx)
        ya = go(a, mine, s_p.at[s, 1], r_p.at[s, 1], at.fy)
        if s > 0:
            far[s][1].wait_recv()
        yb = go(b, mine, s_p.at[s, 2], r_p.at[s, 2], at.fy)
        xb = go(b, mine, s_p.at[s, 3], r_p.at[s, 3], at.fx)
        if s == 0:
            for dz in range(1, depth):
                reach(dz)
        if s == 1:
            near[0][3].wait_recv()
            near[0][4].wait_recv()
            corner = at.z * PLANE + PLANE - 1 - at.spot
            target = at.twin(1) * PLANE + at.spot
            ca = go(a, corner, s_p.at[s, 4], r_p.at[s, 4], target)
            cb = go(b, corner, s_p.at[s, 5], r_p.at[s, 5], target)
            near[0] = near[0][:3]
            near.append((base, xa, ya, yb, xb, ca, cb))
            continue
        xa.wait_recv()
        ra = go(a, base + at.sx, s_p.at[s, 4], r_p.at[s, 4], at.fy)
        yb.wait_recv()
        rb = go(b, base + at.sy, s_p.at[s, 5], r_p.at[s, 5], at.fx)
        near.append((base, ya, xb, ra, rb))
    for base, *group in near:
        for copy in group:
            copy.wait_recv()
        if arrived is not None:
            arrived(base)
    for copy in started:
        copy.wait_send()


def gather_sems(n):
    depth = n // PLANE
    return [DMA((depth, 2)), DMA((depth, 2)), DMA((depth, 6)), DMA((depth, 6))]


def moments(low_rank, first, second):
    first_new = first_decay * first + (1.0 - first_decay) * low_rank
    second_new = second_decay * second + (1.0 - second_decay) * low_rank * low_rank
    ratio = first_new / (jnp.sqrt(second_new) + ratio_floor)
    return (first_new, second_new, ratio)


def wide_dot(narrow, wide):
    total = None
    rest = wide
    for _ in range(3):
        part = rest.astype(jnp.bfloat16)
        rest = rest - part.astype(jnp.float32)
        term = jnp.dot(narrow, part, preferred_element_type=jnp.float32)
        total = term if total is None else total + term
    return total


def main_kernel(
    n,
    m,
    saved_hbm,
    cot_a_hbm,
    cot_b_hbm,
    master_a_hbm,
    master_b_hbm,
    factor_a,
    factor_b,
    first_a,
    second_a,
    first_b,
    second_b,
    step_a,
    step_b,
    first_a_new,
    second_a_new,
    first_b_new,
    second_b_new,
    copy_a_hbm,
    copy_b_hbm,
    saved,
    cot_a,
    cot_b,
    master_a,
    master_b,
    whole_a,
    whole_b,
    mid_a,
    mid_b,
    term_a,
    term_b,
    copy_a,
    copy_b,
    one_a,
    one_b,
    two_a,
    two_b,
    sum_a,
    sum_b,
    ready_a,
    ready_b,
    far_a,
    far_b,
    all_a,
    all_b,
    pair,
    total,
    load_sem,
    store_sem,
    s_mate,
    r_mate,
    s_one,
    r_one,
    s_two,
    r_two,
    s_far,
    r_far,
    fz_s,
    fz_r,
    fp_s,
    fp_r,
    rz_s,
    rz_r,
    rp_s,
    rp_r,
    s_tp,
    r_tp,
    s_fs,
    r_fs,
    cz_s,
    cz_r,
    cp_s,
    cp_r,
):
    at = Place(n)
    depth = at.depth
    t = lax.axis_index("tp")
    others = [lax.rem(at.f + k, n) for k in range(1, n)]
    mates = [lax.rem(t + k, m) for k in range(1, m)]
    loads = [
        pltpu.make_async_copy(src, dst, load_sem.at[k])
        for k, (src, dst) in enumerate(
            (
                (saved_hbm, saved),
                (cot_a_hbm, cot_a),
                (cot_b_hbm, cot_b),
                (master_a_hbm, master_a),
                (master_b_hbm, master_b),
            )
        )
    ]
    for load in loads:
        load.start()
    whole_a[at.f] = factor_a[...]
    whole_b[at.f] = factor_b[...]
    greet([("fs", o) for o in others] + [("tp", o) for o in mates])
    started = []

    def go(copy):
        copy.start()
        started.append(copy)
        return copy

    rows = factor_a.shape[0]
    parts = 2 if m % 2 == 0 else 1
    mate = t + 1 - 2 * lax.rem(t, 2)
    half = pl.ds(pl.multiple_of(lax.rem(t, 2) * (rows // 2), rows // 2), rows // 2) if parts == 2 else pl.ds(0, rows)
    passed = []
    width = PLANE * rows

    def multiply(k):
        base, copies = passed[k]
        for copy in copies:
            copy.wait_recv()
        if k == 0:
            loads[0].wait()
        columns = pl.ds(pl.multiple_of(base * rows, width), width)
        for mid, whole in ((mid_a, whole_a), (mid_b, whole_b)):
            block = whole[pl.ds(base, PLANE)].reshape(width, whole.shape[2])
            product = jnp.dot(saved[:, columns], block, preferred_element_type=jnp.float32)
            if k == 0:
                mid[...] = product
            else:
                mid[...] += product

    def arrived(base):
        k = len(passed)
        copies = []
        if parts == 2:
            for side, whole in enumerate((whole_a, whole_b)):
                view = whole.at[pl.ds(base, PLANE), half]
                copies.append(go(send(view, view, s_mate.at[k, side], r_mate.at[k, side], "tp", mate)))
        passed.append((base, copies))
        if k > 0:
            multiply(k - 1)

    gather(at, whole_a, whole_b, fz_s, fz_r, fp_s, fp_r, lambda ref, index: ref.at[index, half], arrived)
    multiply(depth - 1)

    def project(mid, cot):
        rest = mid[...].T
        result = None
        for _ in range(3):
            part = rest.astype(jnp.bfloat16)
            rest = rest - part.astype(jnp.float32)
            piece = jnp.dot(part, cot[...], preferred_element_type=jnp.float32)
            result = piece if result is None else result + piece
        return result

    loads[1].wait()
    term_a[...] = project(mid_a, cot_a).reshape(term_a.shape)
    first_a_stage = []
    for k in range(depth):
        plane = at.twin(depth - 1 - k)
        first_a_stage.append(
            go(send(term_a.at[plane, :, 1 - at.x], one_a.at[k], s_one.at[k, 0], r_one.at[k, 0], "fs", at.fx))
        )
    loads[2].wait()
    term_b[...] = project(mid_b, cot_b).reshape(term_b.shape)
    first_stage = []
    for k in range(depth):
        plane = at.twin(depth - 1 - k)
        pair_b = go(send(term_b.at[plane, 1 - at.y], one_b.at[k], s_one.at[k, 1], r_one.at[k, 1], "fs", at.fy))
        first_stage.append((first_a_stage[k], pair_b))
    second_stage = []
    third_stage = []
    for k in range(depth + 1):
        if k < depth:
            plane = at.twin(depth - 1 - k)
            first_stage[k][0].wait_recv()
            sum_a[k] = term_a[plane, :, at.x] + one_a[k]
            ca = go(send(sum_a.at[k, 1 - at.y], two_a.at[k], s_two.at[k, 0], r_two.at[k, 0], "fs", at.fy))
            first_stage[k][1].wait_recv()
            sum_b[k] = term_b[plane, at.y] + one_b[k]
            cb = go(send(sum_b.at[k, 1 - at.x], two_b.at[k], s_two.at[k, 1], r_two.at[k, 1], "fs", at.fx))
            second_stage.append((ca, cb))
        if k > 0:
            j = k - 1
            target = at.twin(depth - k) * PLANE + at.spot
            second_stage[j][0].wait_recv()
            ready_a[j] = sum_a[j, at.y] + two_a[j]
            if j < depth - 1:
                ca = go(send(ready_a.at[j], far_a.at[j], s_far.at[j, 0], r_far.at[j, 0], "fs", target))
            second_stage[j][1].wait_recv()
            ready_b[j] = sum_b[j, at.x] + two_b[j]
            if j < depth - 1:
                cb = go(send(ready_b.at[j], far_b.at[j], s_far.at[j, 1], r_far.at[j, 1], "fs", target))
                third_stage.append((ca, cb))
    low_a = ready_a[depth - 1]
    low_b = ready_b[depth - 1]
    for j in range(depth - 1):
        third_stage[j][0].wait_recv()
        low_a = low_a + far_a[j]
        third_stage[j][1].wait_recv()
        low_b = low_b + far_b[j]

    new_first, new_second, ratio = moments(low_a, first_a[...], second_a[...])
    first_a_new[...] = new_first
    second_a_new[...] = new_second
    all_a[at.f] = ratio
    new_first, new_second, ratio = moments(low_b, first_b[...], second_b[...])
    first_b_new[...] = new_first
    second_b_new[...] = new_second
    all_b[at.f] = ratio

    gather(at, all_a, all_b, rz_s, rz_r, rp_s, rp_r)

    rank = all_a.shape[0] * all_a.shape[1]
    cols = all_a.shape[2]
    dir_a = wide_dot(factor_a[...], all_a[...].reshape(rank, cols))
    dir_b = wide_dot(factor_b[...], all_b[...].reshape(rank, cols))
    count = n * dir_a.shape[0] * m * cols

    pair[0, 0:8] = jnp.full((8, 128), jnp.sum(dir_a * dir_a), jnp.float32)
    pair[0, 8:16] = jnp.full((8, 128), jnp.sum(dir_b * dir_b), jnp.float32)
    trips = [
        go(send(pair.at[0], pair.at[k + 1], s_tp.at[k], r_tp.at[k], "tp", mate)) for k, mate in enumerate(mates)
    ]
    step_a[...] = dir_a
    step_b[...] = dir_b
    joint = pair[0]
    for k, trip in enumerate(trips):
        trip.wait_recv()
        joint = joint + pair[k + 1]
    total[0] = joint
    trips = [
        go(send(total.at[0], total.at[k + 1], s_fs.at[k], r_fs.at[k], "fs", other)) for k, other in enumerate(others)
    ]
    joint = total[0]
    for k, trip in enumerate(trips):
        trip.wait_recv()
        joint = joint + total[k + 1]
    scale = lax.rsqrt(joint / count + mean_floor)
    new_step = step_a[...] * scale[0:1, 0:1]
    step_a[...] = new_step
    loads[3].wait()
    copy_a[at.f] = (master_a[...] - step_size * new_step).astype(jnp.bfloat16)
    new_step = step_b[...] * scale[8:9, 0:1]
    step_b[...] = new_step
    loads[4].wait()
    copy_b[at.f] = (master_b[...] - step_size * new_step).astype(jnp.bfloat16)

    stores = []

    def put(base):
        k = len(stores)
        block = pl.ds(base, PLANE)
        for side, (src, dst) in enumerate(((copy_a, copy_a_hbm), (copy_b, copy_b_hbm))):
            stores.append(pltpu.make_async_copy(src.at[block], dst.at[block], store_sem.at[k + side]))
            stores[-1].start()

    gather(at, copy_a, copy_b, cz_s, cz_r, cp_s, cp_r, whole_block, put)
    for store in stores:
        store.wait()
    for copy in started:
        copy.wait_send()


def hand_kernel(depth, *refs):
    count = (len(refs) - 2) // 3
    given, out, held = refs[:count], refs[count : 2 * count], refs[2 * count : 3 * count]
    in_sem, out_sem = refs[3 * count :]
    moves = []
    for k in range(count):
        pieces = depth if len(given[k].shape) == 3 else 1
        size = given[k].shape[0] // pieces
        for i in range(pieces):
            part = pl.ds(i * size, size)
            moves.append(
                (
                    pltpu.make_async_copy(given[k].at[part], held[k].at[part], in_sem.at[k, i]),
                    pltpu.make_async_copy(held[k].at[part], out[k].at[part], out_sem.at[k, i]),
                )
            )
    for into, _ in moves:
        into.start()
    for into, onward in moves:
        into.wait()
        onward.start()
    for _, onward in moves:
        onward.wait()


def local(
    n,
    m,
    saved_inputs,
    input_cot,
    gate_cot,
    input_master,
    gate_master,
    input_factor,
    gate_factor,
    input_first,
    input_second,
    gate_first,
    gate_second,
):
    in_vmem = pl.BlockSpec(memory_space=VMEM)
    anywhere = pl.BlockSpec(memory_space=pl.ANY)
    rows, rank = input_factor.shape
    tokens = saved_inputs.shape[0]
    low_rows, cols = input_first.shape
    depth = n // PLANE
    shape = jax.ShapeDtypeStruct
    f32, bf16 = jnp.float32, jnp.bfloat16
    low = shape((low_rows, cols), f32)
    piece = (low_rows, cols)
    full = shape((rows, cols), f32)
    copies = shape((n, rows, cols), bf16)
    shapes = [full, full, low, low, low, low, copies, copies]
    outs = pl.pallas_call(
        functools.partial(main_kernel, n, m),
        out_shape=shapes,
        in_specs=[anywhere] * 5 + [in_vmem] * 6,
        out_specs=[in_vmem] * 6 + [anywhere] * 2,
        scratch_shapes=[
            VMEM(saved_inputs.shape, bf16),
            VMEM(input_cot.shape, bf16),
            VMEM(input_cot.shape, bf16),
            VMEM((rows, cols), f32),
            VMEM((rows, cols), f32),
            VMEM((n, rows, rank), bf16),
            VMEM((n, rows, rank), bf16),
            VMEM((tokens, rank), f32),
            VMEM((tokens, rank), f32),
            VMEM((depth, 2, 2) + piece, f32),
            VMEM((depth, 2, 2) + piece, f32),
            VMEM((n, rows, cols), bf16),
            VMEM((n, rows, cols), bf16),
            VMEM((depth, 2) + piece, f32),
            VMEM((depth, 2) + piece, f32),
            VMEM((depth,) + piece, f32),
            VMEM((depth,) + piece, f32),
            VMEM((depth, 2) + piece, f32),
            VMEM((depth, 2) + piece, f32),
            VMEM((depth,) + piece, f32),
            VMEM((depth,) + piece, f32),
            VMEM((depth,) + piece, f32),
            VMEM((depth,) + piece, f32),
            VMEM((n,) + piece, f32),
            VMEM((n,) + piece, f32),
            VMEM((m, 16, 128), f32),
            VMEM((n, 16, 128), f32),
            DMA((5,)),
            DMA((2 * depth,)),
            *[DMA((depth, 2))] * 8,
            *gather_sems(n),
            *gather_sems(n),
            DMA((m,)),
            DMA((m,)),
            DMA((n,)),
            DMA((n,)),
            *gather_sems(n),
        ],
        compiler_params=pltpu.CompilerParams(
            collective_id=1, has_side_effects=True, vmem_limit_bytes=56 * 2**20
        ),
        name="update",
    )(
        saved_inputs,
        input_cot,
        gate_cot,
        input_master,
        gate_master,
        input_factor,
        gate_factor,
        input_first,
        input_second,
        gate_first,
        gate_second,
    )
    outs = pl.pallas_call(
        functools.partial(hand_kernel, depth),
        out_shape=shapes,
        in_specs=[anywhere] * 8,
        out_specs=[anywhere] * 8,
        scratch_shapes=[VMEM(s.shape, s.dtype) for s in shapes] + [DMA((8, depth))] * 2,
        name="results",
    )(*outs)
    *head, copy_in, copy_gate = outs
    return (*head, copy_in.reshape(n * rows, cols), copy_gate.reshape(n * rows, cols))


def solution(mesh):
    n, m = mesh.shape["fs"], mesh.shape["tp"]
    both = P("fs", "tp")
    rows = P("fs", None)
    return jax.shard_map(
        functools.partial(local, n, m),
        mesh=mesh,
        in_specs=(rows, both, both, both, both, rows, rows, both, both, both, both),
        out_specs=(both,) * 6 + (P(None, "tp"),) * 2,
        check_vma=False,
    )
```
